256 devices in a mesh: ep: 128 (over z, y, x), tp: 2 (over core).
Axes of the slice: x: 4, y: 4, z: 8, core: 2. Of those that a mesh axis runs over, the one named last changes fastest.
Arguments:
- tokens: bfloat16 [2048, 2048], P('ep', 'tp'), may hold values from -6 to 6
- lengths: int32 [2048], P('ep'), may hold values from 1 to 1024
- lat_cache: bfloat16 [2048, 1024, 256], P(('ep', 'tp')), may hold values from -6 to 6
- rope_cache: bfloat16 [2048, 1024, 32], P(('ep', 'tp'))
- norm1_gain: float32 [2048], replicated, may hold values from 0.1 to 1.9
- w_qdown: bfloat16 [2048, 512], P('tp'), may hold values from -0.125 to 0.125
- w_kvdown: bfloat16 [2048, 256], P('tp'), may hold values from -0.125 to 0.125
- w_kdown_rope: bfloat16 [2048, 32], P('tp'), may hold values from -0.125 to 0.125
- qnorm_gain: float32 [512], replicated, may hold values from 0.1 to 1.9
- kvnorm_gain: float32 [256], replicated, may hold values from 0.1 to 1.9
- w_qup_nope: bfloat16 [512, 16, 64], P(None, 'tp'), may hold values from -0.25 to 0.25
- w_qup_rope: bfloat16 [512, 16, 32], P(None, 'tp'), may hold values from -0.25 to 0.25
- w_absorb_k: bfloat16 [16, 64, 256], P('tp'), may hold values from -0.75 to 0.75
- w_absorb_v: bfloat16 [16, 256, 64], P('tp'), may hold values from -0.375 to 0.375
- w_attn_out: bfloat16 [16, 64, 2048], P('tp'), may hold values from -0.1875 to 0.1875
- norm2_gain: float32 [2048], replicated, may hold values from 0.1 to 1.9
- routes: int32 [2048, 6], P('ep'), may hold values from 0 to 127, all different within a row; in each aligned block of 16 rows (0 to 15, 16 to 31, ...) at most 2 rows name the same one
- route_weights: float32 [2048, 6], P('ep'), may hold values from 0.1 to 1
- w_exp_gate: bfloat16 [128, 2048, 512], P('ep', None, 'tp'), may hold values from -0.125 to 0.125
- w_exp_up: bfloat16 [128, 2048, 512], P('ep', None, 'tp'), may hold values from -0.125 to 0.125
- w_exp_down: bfloat16 [128, 512, 2048], P('ep', 'tp'), may hold values from -0.25 to 0.25
Outputs:
- mixed: bfloat16 [2048, 2048], P('ep', 'tp')
- new_latent: bfloat16 [2048, 256], P(('ep', 'tp'))
- new_rope_key: bfloat16 [2048, 32], P(('ep', 'tp'))
The draws below stay inside these ranges and needn't reach their ends.
Inputs may be any that keep to these rules, and one draw needn't show every extreme that they name: `routes`: each row names 6 different experts; the 16 rows of one index of ep name one expert at most 2 times, and some expert exactly so often. `lengths`: the new token's position; cached positions from it on are not in use.
All inputs are finite; a program needn't handle non-finite values.
Results may differ from the reference program's by a relative error of at most 0.015.
Values may be sent and summed in bfloat16 or wider, within the bound.
A program may use at most 64 MiB of HBM per device.

```python
import math
from functools import partial
import jax
import jax.numpy as jnp
import numpy as np
from jax import lax

D = 2048
HEADS = 16
NOPE = 64
ROPE_DIM = 32
VDIM = 64
QRANK = 512
KVRANK = 256
EXP_HID = 512
TOP_K = 6
SEQ_GRP = 16
CACHE = 1024
SEQS = 2048
EXPERTS = 128
CAPACITY = 2
N_EP = 128


def draw_rope_cache(key, part):
    values = jax.random.normal(jax.random.fold_in(key, 11), (SEQS, CACHE, ROPE_DIM), jnp.float32)
    return values.astype(jnp.bfloat16)


def touch_ends(drawn, key, smallest, largest):
    shape = drawn.shape
    index_at = [jax.random.randint(jax.random.fold_in(key, axis), (), 0, shape[axis]) for axis in range(len(shape))]
    drawn = drawn.at[tuple(index_at)].set(smallest)
    longest = shape.index(max(shape))
    index_at[longest] = (index_at[longest] + 1) % shape[longest]
    return drawn.at[tuple(index_at)].set(largest)


def block_scale(own_key, shape, split, least, high):
    factor_of = 1.0
    for axis_at, parts in split:
        heights = jax.random.uniform(jax.random.fold_in(jax.random.fold_in(own_key, 6), axis_at), (parts,), jnp.float32, least / len(split), high / len(split))
        factor_of = factor_of * jnp.repeat(jnp.exp(heights), shape[axis_at] // parts).reshape((-1,) + (1,) * (len(shape) - 1 - axis_at))
    return factor_of


def shared_out(key, own, number, rows, count, top, most, lean):
    sequence = jax.random.permutation(key, count)
    packed, usual = shares(count, rows * top, most, lean, True), shares(count, rows * top, most, lean, False)
    places = jnp.arange(count)

    def named(sizes, rotation):
        used = int((sizes > 0).sum())
        fixed = max(1, used // 4)
        passed = fixed + (places - fixed + rotation * (used - fixed)) % max(1, count - fixed)
        return jnp.zeros((count,), jnp.int32).at[sequence[jnp.where(places < fixed, places, passed)]].set(jnp.asarray(sizes, jnp.int32))

    sizes = jnp.where(number % 4 == 0, named(packed, number // 4), named(usual, number - number // 4 - 1))
    mixed = jax.random.permutation(jax.random.fold_in(own, 3), count)
    donor, sink = mixed[0:count // 2 * 2:2], mixed[1:count // 2 * 2:2]
    room = jnp.minimum(sizes[donor] - 1, most - sizes[sink]) // 2
    room = jnp.where((donor == sequence[0]) | (sink == sequence[0]) | (sizes[sink] == 0), 0, jnp.maximum(room, 0))
    passed = jax.random.randint(jax.random.fold_in(own, 4), (count // 2,), 0, 1 << 20) % (room + 1)
    sizes = sizes.at[donor].add(-passed).at[sink].add(passed)
    labels = jnp.searchsorted(jnp.cumsum(sizes), jnp.arange(rows * top), side="right").astype(jnp.int32)
    listing = labels.reshape(top, rows).T
    listing = listing[jax.random.permutation(jax.random.fold_in(own, 1), rows)]
    rotation = jax.random.randint(jax.random.fold_in(own, 2), (rows, 1), 0, top)
    return jnp.take_along_axis(listing, (jnp.arange(top)[None, :] + rotation) % top, axis=1)


def shares(amount, total, bound, lean, full):
    weights = [(1 << 20) // math.isqrt(standing ** lean) + 1 for standing in range(1, amount + 1)]
    largest = bound if full else min(bound, max(-(-total // amount), total * weights[0] // sum(weights)))
    least = 1 if total - largest >= amount - 1 else 0
    holding, surplus = [largest] + [least] * (amount - 1), total - largest - least * (amount - 1)
    while surplus > 0:
        movable = [i for i in range(1, amount) if holding[i] < largest] or [i for i in range(1, amount) if holding[i] < bound]
        mass, left = sum([weights[i] for i in movable]), surplus
        for i in movable:
            extra = min(bound - holding[i], max(1, left * weights[i] // mass), surplus)
            holding[i] = holding[i] + extra
            surplus = surplus - extra
    return np.array(holding)


def scatter_about(own_key, shape, deviation, reach, pieces=(), held_as=jnp.bfloat16):
    result = deviation * jax.random.normal(own_key, shape, jnp.float32)
    if pieces:
        result = result * block_scale(own_key, shape, pieces, -0.22, 0.18)
    return jnp.clip(result, -reach, reach).astype(held_as)


def setup_inputs(seed: int = 0) -> dict:
    arg_keys = jax.random.split(jax.random.key(seed), 22)
    tokens = scatter_about(arg_keys[0], (SEQS, D), 1.0, 6.0, ((0, 128), (1, 2)))
    lengths = touch_ends(jax.random.randint(arg_keys[1], (SEQS,), 1, CACHE + 1), jax.random.fold_in(arg_keys[1], 1), 1, CACHE).astype(jnp.int32)
    lat_cache = scatter_about(arg_keys[2], (SEQS, CACHE, KVRANK), 1.0, 6.0, ((0, 256),))
    rope_cache = draw_rope_cache(jax.random.fold_in(arg_keys[21], 71), 0)
    norm1_gain = jnp.clip(1.0 + 0.18 * jax.random.normal(arg_keys[4], (D,), jnp.float32), 0.1, 1.9)
    w_qdown = scatter_about(arg_keys[5], (D, QRANK), D ** -0.5, 0.125, ((0, 2),))
    w_kvdown = scatter_about(arg_keys[6], (D, KVRANK), D ** -0.5, 0.125, ((0, 2),))
    w_kdown_rope = scatter_about(arg_keys[7], (D, ROPE_DIM), D ** -0.5, 0.125, ((0, 2),))
    qnorm_gain = jnp.clip(1.0 + 0.18 * jax.random.normal(arg_keys[8], (QRANK,), jnp.float32), 0.1, 1.9)
    kvnorm_gain = jnp.clip(1.0 + 0.18 * jax.random.normal(arg_keys[9], (KVRANK,), jnp.float32), 0.1, 1.9)
    w_qup_nope = scatter_about(arg_keys[10], (QRANK, HEADS, NOPE), QRANK ** -0.5, 0.25, ((1, 2),))
    w_qup_rope = scatter_about(arg_keys[11], (QRANK, HEADS, ROPE_DIM), QRANK ** -0.5, 0.25, ((1, 2),))
    w_absorb_k = scatter_about(arg_keys[12], (HEADS, NOPE, KVRANK), NOPE ** -0.5, 0.75, ((0, 2),))
    w_absorb_v = scatter_about(arg_keys[13], (HEADS, KVRANK, VDIM), KVRANK ** -0.5, 0.375, ((0, 2),))
    w_attn_out = scatter_about(arg_keys[14], (HEADS, VDIM, D), (HEADS * VDIM) ** -0.5, 0.1875, ((0, 2),))
    norm2_gain = jnp.clip(1.0 + 0.18 * jax.random.normal(arg_keys[15], (D,), jnp.float32), 0.1, 1.9)
    routes_keys = jax.random.split(jax.random.fold_in(arg_keys[16], 1), SEQS // SEQ_GRP)
    routes_turns = jax.random.permutation(jax.random.fold_in(arg_keys[16], 3), SEQS // SEQ_GRP)
    routes = jax.vmap(lambda own, number: shared_out(jax.random.fold_in(arg_keys[16], 2), own, number, SEQ_GRP, EXPERTS, TOP_K, CAPACITY, 2))(routes_keys, routes_turns).reshape((SEQS, TOP_K))
    route_weights = jnp.clip(jnp.exp(math.log(1.0) - 2.3025851 * jax.random.uniform(arg_keys[17], (SEQS, TOP_K), jnp.float32) ** block_scale(arg_keys[17], (SEQS, TOP_K), ((0, 128),), -0.2, 0.2)), 0.1, 1.0)
    w_exp_gate = scatter_about(arg_keys[18], (EXPERTS, D, EXP_HID), D ** -0.5, 0.125, ((0, 128), (2, 2)))
    w_exp_up = scatter_about(arg_keys[19], (EXPERTS, D, EXP_HID), D ** -0.5, 0.125, ((0, 128), (2, 2)))
    w_exp_down = scatter_about(arg_keys[20], (EXPERTS, EXP_HID, D), EXP_HID ** -0.5, 0.25, ((0, 128), (1, 2)))
    return {"tokens": tokens, "lengths": lengths, "lat_cache": lat_cache, "rope_cache": rope_cache, "norm1_gain": norm1_gain, "w_qdown": w_qdown, "w_kvdown": w_kvdown, "w_kdown_rope": w_kdown_rope, "qnorm_gain": qnorm_gain, "kvnorm_gain": kvnorm_gain, "w_qup_nope": w_qup_nope, "w_qup_rope": w_qup_rope, "w_absorb_k": w_absorb_k, "w_absorb_v": w_absorb_v, "w_attn_out": w_attn_out, "norm2_gain": norm2_gain, "routes": routes, "route_weights": route_weights, "w_exp_gate": w_exp_gate, "w_exp_up": w_exp_up, "w_exp_down": w_exp_down}


rms_eps = 1e-06
rope_base = 10000.0

def rms_scale(values, gain_vector):
    mean_square = lax.optimization_barrier(jnp.mean(values * values, axis=-1, keepdims=True))
    return values * lax.rsqrt(mean_square + rms_eps) * gain_vector

def rotate(values, positions):
    half_size = values.shape[-1] // 2
    frequency = jnp.exp(-jnp.log(rope_base) * jnp.arange(half_size, dtype=jnp.float32) / half_size)
    angles = positions.astype(jnp.float32)[:, None] * frequency[None, :]
    view_shape = (angles.shape[0],) + (1,) * (values.ndim - 2) + (half_size,)
    cosine = jnp.cos(angles).reshape(view_shape)
    sine_part = jnp.sin(angles).reshape(view_shape)
    first_half = values[..., :half_size]
    second_half = values[..., half_size:]
    return jnp.concatenate([first_half * cosine - second_half * sine_part, second_half * cosine + first_half * sine_part], -1)

def slot_tables(group_routes, group_weights, experts, capacity):
    row_count, top_count = group_routes.shape
    flat_routes = group_routes.reshape(-1)
    matches = (flat_routes[:, None] == jnp.arange(experts, dtype=jnp.int32)[None, :]).astype(jnp.int32)
    earlier = jnp.cumsum(matches, axis=0) - matches
    slot_index = lax.optimization_barrier(jnp.sum(earlier * matches, axis=1))
    target = flat_routes * capacity + slot_index
    slot_match = (target[:, None] == jnp.arange(experts * capacity, dtype=jnp.int32)[None, :]).astype(jnp.float32)
    slot_match = slot_match.reshape(row_count, top_count, experts * capacity)
    dispatch = lax.optimization_barrier(jnp.sum(slot_match, axis=1)).T
    weighing = lax.optimization_barrier(jnp.sum(slot_match * group_weights[:, :, None], axis=1))
    return (dispatch, weighing)

def attend_group(block_items):
    query_latent, query_rope, latents, rope_keys, fresh_latent, fresh_rope, own_lengths = block_items
    latent_f = latents.astype(jnp.float32)
    past_scores = jnp.einsum('shc,spc->shp', query_latent.astype(jnp.float32), latent_f)
    past_scores = past_scores + jnp.einsum('shr,spr->shp', query_rope.astype(jnp.float32), rope_keys.astype(jnp.float32))
    cache_positions = lax.broadcasted_iota(jnp.int32, past_scores.shape, 2)
    live_mask = cache_positions < own_lengths[:, None, None]
    past_scores = jnp.where(live_mask, past_scores, -jnp.inf)
    own_score = jnp.einsum('shc,sc->sh', query_latent.astype(jnp.float32), fresh_latent.astype(jnp.float32))
    own_score = own_score + jnp.einsum('shr,sr->sh', query_rope.astype(jnp.float32), fresh_rope.astype(jnp.float32))
    row_peak = jnp.maximum(lax.optimization_barrier(jnp.max(past_scores, axis=2)), own_score)
    past_weights = jnp.exp(past_scores - row_peak[:, :, None])
    own_weight = jnp.exp(own_score - row_peak)
    denominator = lax.optimization_barrier(jnp.sum(past_weights, axis=2)) + own_weight
    past_probs = (past_weights / denominator[:, :, None]).astype(jnp.bfloat16)
    own_prob = (own_weight / denominator).astype(jnp.bfloat16)
    mixed_latent = jnp.einsum('shp,spc->shc', past_probs.astype(jnp.float32), latent_f)
    mixed_latent = mixed_latent + own_prob.astype(jnp.float32)[:, :, None] * fresh_latent.astype(jnp.float32)[:, None, :]
    return mixed_latent.astype(jnp.bfloat16)

def reference(tokens, lengths, lat_cache, rope_cache, norm1_gain, w_qdown, w_kvdown, w_kdown_rope, qnorm_gain, kvnorm_gain, w_qup_nope, w_qup_rope, w_absorb_k, w_absorb_v, w_attn_out, norm2_gain, routes, route_weights, w_exp_gate, w_exp_up, w_exp_down):
    score_scale = (w_qup_nope.shape[2] + w_qup_rope.shape[2]) ** (-0.5)
    token_values = tokens.astype(jnp.float32)
    normed1 = rms_scale(token_values, norm1_gain).astype(jnp.bfloat16)
    query_low = jnp.dot(normed1, w_qdown, preferred_element_type=jnp.float32)
    kv_low = jnp.dot(normed1, w_kvdown, preferred_element_type=jnp.float32)
    rope_low = jnp.dot(normed1, w_kdown_rope, preferred_element_type=jnp.float32)
    compressed = rms_scale(query_low, qnorm_gain).astype(jnp.bfloat16)
    new_latent = rms_scale(kv_low, kvnorm_gain).astype(jnp.bfloat16)
    new_rope_key = rotate(rope_low, lengths).astype(jnp.bfloat16)
    compressed_f = compressed.astype(jnp.float32)
    query_nope = jnp.einsum('sc,chd->shd', compressed_f, w_qup_nope.astype(jnp.float32)).astype(jnp.bfloat16)
    rope_part = jnp.einsum('sc,chd->shd', compressed_f, w_qup_rope.astype(jnp.float32))
    query_rope = (rotate(rope_part, lengths) * score_scale).astype(jnp.bfloat16)
    query_latent = (jnp.einsum('shd,hdc->shc', query_nope.astype(jnp.float32), w_absorb_k.astype(jnp.float32)) * score_scale).astype(jnp.bfloat16)

    def grouped(array):
        return array.reshape((N_EP, SEQ_GRP) + array.shape[1:])
    attended = lax.map(attend_group, (grouped(query_latent), grouped(query_rope), grouped(lat_cache), grouped(rope_cache), grouped(new_latent), grouped(new_rope_key), grouped(lengths)))
    attended = attended.reshape((SEQS,) + attended.shape[2:])
    head_out = jnp.einsum('shc,hcv->shv', attended.astype(jnp.float32), w_absorb_v.astype(jnp.float32)).astype(jnp.bfloat16)
    attention_sum = jnp.einsum('shv,hvd->sd', head_out.astype(jnp.float32), w_attn_out.astype(jnp.float32))
    hidden1 = (token_values + attention_sum).astype(jnp.bfloat16)
    normed2 = rms_scale(hidden1.astype(jnp.float32), norm2_gain).astype(jnp.bfloat16)
    tables = jax.vmap(partial(slot_tables, experts=EXPERTS, capacity=CAPACITY))
    dispatch, weighing = tables(grouped(routes), grouped(route_weights))
    sent_rows = jnp.einsum('gms,gsd->gmd', dispatch, grouped(normed2).astype(jnp.float32))
    by_expert = sent_rows.reshape(N_EP, EXPERTS, CAPACITY, D).transpose(1, 0, 2, 3).reshape(EXPERTS, N_EP * CAPACITY, D).astype(jnp.bfloat16)

    def run_expert(expert_item):
        expert_rows, gate_matrix, up_matrix, down_matrix = expert_item
        gate_value = jnp.dot(expert_rows, gate_matrix, preferred_element_type=jnp.float32)
        up_value = jnp.dot(expert_rows, up_matrix, preferred_element_type=jnp.float32)
        expert_hidden = (jax.nn.silu(gate_value) * up_value).astype(jnp.bfloat16)
        return jnp.dot(expert_hidden, down_matrix, preferred_element_type=jnp.float32).astype(jnp.bfloat16)
    expert_outputs = lax.map(run_expert, (by_expert, w_exp_gate, w_exp_up, w_exp_down))
    returned = expert_outputs.reshape(EXPERTS, N_EP, CAPACITY, D).transpose(1, 0, 2, 3).reshape(N_EP, EXPERTS * CAPACITY, D)
    routed = jnp.einsum('gsm,gmd->gsd', weighing, returned.astype(jnp.float32)).reshape(SEQS, D)
    mixed = (hidden1.astype(jnp.float32) + routed).astype(jnp.bfloat16)
    return (mixed, new_latent, new_rope_key)
```

```python
import jax
import jax.numpy as jnp
from jax import lax
from jax.experimental import pallas as pl
from jax.experimental.pallas import tpu as pltpu
from jax.sharding import PartitionSpec as P

rms_eps = 1e-06
rope_base = 10000.0


def laid_out(blocks, dim):
    shape = list(blocks.shape[1:])
    shape[dim] *= blocks.shape[0]
    return jnp.moveaxis(blocks, 0, dim).reshape(shape)


def from_everyone(array, axis):
    size = lax.axis_size(axis)
    return lax.all_to_all(
        jnp.broadcast_to(array[None], (size, *array.shape)), axis, 0, 0, tiled=True
    )


def gather_directly(array, axis, dim):
    return laid_out(from_everyone(array, axis), dim)


def over_copies(array, axis):
    everything = from_everyone(array, axis)
    return jnp.sum(everything, axis=0)


def in_one(arrays, axis):
    vector, at, outs = (jnp.concatenate([a.reshape(-1) for a in arrays]), 0, [])
    running = over_copies(vector, axis)
    for a in arrays:
        outs.append(running[at : at + a.size].reshape(a.shape))
        at += a.size
    return tuple(outs)


def sent_together(arrays, axis, split_dim, concat_dim, along):
    ends, at = ([], 0)
    for a in arrays[:-1]:
        at += a.shape[along]
        ends.append(at)
    both = jnp.concatenate(arrays, axis=along)
    return tuple(
        jnp.split(
            lax.all_to_all(both, axis, split_axis=split_dim, concat_axis=concat_dim, tiled=True),
            ends,
            axis=along,
        )
    )


def rms_scale(values, gain_vector):
    mean_square = jnp.mean(values * values, axis=-1, keepdims=True)
    return values * lax.rsqrt(mean_square + rms_eps) * gain_vector


def rotate(values, positions):
    half_size = values.shape[-1] // 2
    frequency = jnp.exp(-jnp.log(rope_base) * jnp.arange(half_size, dtype=jnp.float32) / half_size)
    angles = positions.astype(jnp.float32)[:, None] * frequency[None, :]
    view_shape = (angles.shape[0],) + (1,) * (values.ndim - 2) + (half_size,)
    cosine = jnp.cos(angles).reshape(view_shape)
    sine_part = jnp.sin(angles).reshape(view_shape)
    first_half = values[..., :half_size]
    second_half = values[..., half_size:]
    return jnp.concatenate(
        [
            first_half * cosine - second_half * sine_part,
            second_half * cosine + first_half * sine_part,
        ],
        -1,
    )


def attend(query_latent, query_rope, latents, rope_keys, fresh_latent, fresh_rope, own_lengths):
    past_scores = jnp.einsum(
        "shc,spc->shp", query_latent, latents, preferred_element_type=jnp.float32
    )
    past_scores = past_scores + jnp.einsum(
        "shr,spr->shp", query_rope, rope_keys, preferred_element_type=jnp.float32
    )
    cache_positions = lax.broadcasted_iota(jnp.int32, past_scores.shape, 2)
    past_scores = jnp.where(cache_positions < own_lengths[:, None, None], past_scores, -jnp.inf)
    own_score = jnp.einsum(
        "shc,sc->sh", query_latent, fresh_latent, preferred_element_type=jnp.float32
    )
    own_score = own_score + jnp.einsum(
        "shr,sr->sh", query_rope, fresh_rope, preferred_element_type=jnp.float32
    )
    row_peak = jnp.maximum(jnp.max(past_scores, axis=2), own_score)
    past_weights = jnp.exp(past_scores - row_peak[:, :, None])
    own_weight = jnp.exp(own_score - row_peak)
    denominator = jnp.sum(past_weights, axis=2) + own_weight
    past_probs = (past_weights / denominator[:, :, None]).astype(jnp.bfloat16)
    own_prob = (own_weight / denominator).astype(jnp.bfloat16)
    mixed_latent = jnp.einsum(
        "shp,spc->shc", past_probs, latents, preferred_element_type=jnp.float32
    )
    mixed_latent = (
        mixed_latent
        + own_prob.astype(jnp.float32)[:, :, None] * fresh_latent.astype(jnp.float32)[:, None, :]
    )
    return mixed_latent.astype(jnp.bfloat16)


mesh_ids = pl.DeviceIdType.MESH
plane_size = 16
group_rows = 16


def remote(src, dst, send_sem, recv_sem, chip, core):
    return pltpu.make_async_remote_copy(
        src_ref=src,
        dst_ref=dst,
        send_sem=send_sem,
        recv_sem=recv_sem,
        device_id={"ep": chip, "tp": core},
        device_id_type=mesh_ids,
    )


def rows_at(index):
    return pl.ds(pl.multiple_of(index * group_rows, group_rows), group_rows)


def half_at(core, width):
    return pl.ds(pl.multiple_of(core * width, width), width)


def greet(depth):
    me, core = lax.axis_index("ep"), lax.axis_index("tp")
    layer, spot = me // plane_size, lax.rem(me, plane_size)
    barrier = pltpu.get_barrier_semaphore()

    def signal(chip, to_core):
        pl.semaphore_signal(
            barrier, inc=1, device_id={"ep": chip, "tp": to_core}, device_id_type=mesh_ids
        )

    signal(me, 1 - core)

    def in_column(k, carry):
        signal(lax.rem(layer + k, depth) * plane_size + spot, core)
        return carry

    def in_plane(k, carry):
        chip = layer * plane_size + lax.rem(spot + k, plane_size)
        signal(chip, core)
        signal(chip, 1 - core)
        return carry

    lax.fori_loop(1, depth, in_column, 0)
    lax.fori_loop(1, plane_size, in_plane, 0)
    pl.semaphore_wait(barrier, 1 + (depth - 1) + 2 * (plane_size - 1))


def place_routes(routes_ref, weights_ref, table_buf, layer, depth):
    lanes = lax.broadcasted_iota(jnp.int32, (routes_ref.shape[0], depth * group_rows), 1)
    own = lanes // group_rows == layer
    spread = jnp.concatenate([routes_ref[...].astype(jnp.float32)] * depth, axis=1)
    spread_weights = jnp.concatenate([weights_ref[...]] * depth, axis=1)
    top_count = routes_ref.shape[0]
    table_buf[layer] = jnp.zeros(table_buf.shape[1:], jnp.float32)
    table_buf[layer, 0:top_count] = jnp.where(own, spread, 0.0)
    table_buf[layer, 8 : 8 + top_count] = jnp.where(own, spread_weights, 0.0)


def tables(table_buf, layer, top_count):
    table = jnp.sum(table_buf[...], axis=0)
    token_count = table.shape[1]
    shape = (plane_size * group_rows, token_count)
    rows = lax.broadcasted_iota(jnp.int32, shape, 0)
    lanes = lax.broadcasted_iota(jnp.int32, shape, 1)
    expert = (layer * plane_size + rows // group_rows).astype(jnp.float32)
    hit = jnp.zeros(shape, jnp.float32)
    weight = jnp.zeros(shape, jnp.float32)
    for k in range(top_count):
        named = expert == table[k : k + 1]
        hit = jnp.where(named, 1.0, hit)
        weight = jnp.where(named, table[8 + k : 9 + k], weight)
    same_group = lanes // group_rows == lax.rem(rows, group_rows) // 2
    hit = jnp.where(same_group, hit, 0.0)
    square = (token_count, token_count)
    before = lax.broadcasted_iota(jnp.int32, square, 0) < lax.broadcasted_iota(
        jnp.int32, square, 1
    )
    earlier = jnp.dot(
        hit.astype(jnp.bfloat16),
        jnp.where(before, 1.0, 0.0).astype(jnp.bfloat16),
        preferred_element_type=jnp.float32,
    )
    chosen = (hit > 0.5) & (earlier == lax.rem(rows, 2).astype(jnp.float32))
    dispatch = jnp.where(chosen, 1.0, 0.0).astype(jnp.bfloat16)
    weighing = jnp.where(chosen, weight, 0.0).T.astype(jnp.bfloat16)
    return dispatch, weighing


def send_in_column(buf, slot_shape_at, send_sems, recv_sems, depth, source=None):
    me, core = lax.axis_index("ep"), lax.axis_index("tp")
    layer, spot = me // plane_size, lax.rem(me, plane_size)
    for k in (4, 3, 5, 2, 6, 1, 7):
        peer = lax.rem(layer + k, depth)
        src = slot_shape_at(buf, layer) if source is None else slot_shape_at(source, peer)
        remote(
            src,
            slot_shape_at(buf, layer),
            send_sems.at[k],
            recv_sems.at[layer],
            peer * plane_size + spot,
            core,
        ).start()


def column_waits(buf, slot_shape_at, send_sems, recv_sems, depth, sends):
    me, core = lax.axis_index("ep"), lax.axis_index("tp")
    layer, spot = me // plane_size, lax.rem(me, plane_size)
    for k in (1, 7, 2, 6, 3, 5, 4):
        peer = lax.rem(layer + k, depth)
        copy = remote(
            slot_shape_at(buf, peer),
            slot_shape_at(buf, peer),
            send_sems.at[k],
            recv_sems.at[peer],
            peer * plane_size + spot,
            core,
        )
        if sends:
            copy.wait_send()
        else:
            copy.wait_recv()


def moe_kernel(
    x_ref,
    hidden_ref,
    routes_ref,
    weights_ref,
    gate_hbm,
    up_hbm,
    down_hbm,
    out_ref,
    gate,
    up,
    down,
    table_buf,
    x_buf,
    d_send,
    r_buf,
    y_send,
    y_buf,
    p_send,
    p_buf,
    load_sems,
    w_send,
    w_recv,
    t_send,
    t_recv,
    x_send_sem,
    x_recv,
    d_send_sem,
    d_recv,
    y_send_sem,
    y_recv,
    p_send_sem,
    p_recv,
):
    depth = table_buf.shape[0]
    me, core = lax.axis_index("ep"), lax.axis_index("tp")
    layer, spot = me // plane_size, lax.rem(me, plane_size)
    half = x_ref.shape[1]
    mine = lax.rem(spot, 2) == core
    loads = [
        pltpu.make_async_copy(src.at[0], dst.at[0], load_sems.at[n])
        for n, (src, dst) in enumerate(((gate_hbm, gate), (up_hbm, up), (down_hbm, down)))
    ]
    for load in loads:
        load.start()
    place_routes(routes_ref, weights_ref, table_buf, layer, depth)
    x_buf[rows_at(layer)] = x_ref[...]
    greet(depth)

    def tile_at(buf, slot):
        return buf.at[slot]

    def block_at(buf, slot):
        return buf.at[rows_at(slot)]

    send_in_column(table_buf, tile_at, t_send, t_recv, depth)
    send_in_column(x_buf, block_at, x_send_sem, x_recv, depth)
    swaps = [
        remote(src.at[0], dst.at[1], w_send.at[n], w_recv.at[n], me, 1 - core)
        for n, (src, dst) in enumerate(((gate_hbm, gate), (up_hbm, up), (down_hbm, down)))
    ]
    for swap in swaps:
        swap.start()
    column_waits(table_buf, tile_at, t_send, t_recv, depth, False)
    dispatch, weighing = tables(table_buf, layer, routes_ref.shape[0])
    column_waits(x_buf, block_at, x_send_sem, x_recv, depth, False)
    d_send[...] = jnp.dot(dispatch, x_buf[...], preferred_element_type=jnp.float32).astype(
        jnp.bfloat16
    )

    def row_copy(spot_to, spot_from, core_from):
        return remote(
            d_send.at[rows_at(spot_to)],
            r_buf.at[rows_at(spot_from // 2), half_at(core_from, half)],
            d_send_sem.at[spot_to],
            d_recv.at[spot_from // 2, core_from],
            layer * plane_size + spot_to,
            lax.rem(spot_from, 2),
        )

    def send_rows(n, carry):
        spot_to = spot ^ (15 - n)

        @pl.when((spot_to != spot) | jnp.logical_not(mine))
        def _():
            row_copy(spot_to, spot, core).start()

        return carry

    lax.fori_loop(0, plane_size, send_rows, 0)

    @pl.when(mine)
    def _():
        r_buf[rows_at(spot // 2), half_at(core, half)] = d_send[rows_at(spot)]

    def recv_rows(n, carry):
        spot_from = spot ^ (2 * (n // 2) + (lax.rem(spot, 2) ^ core))
        core_from = lax.rem(n, 2)

        @pl.when((spot_from != spot) | (core_from != core))
        def _():
            remote(
                d_send.at[rows_at(0)],
                r_buf.at[rows_at(spot_from // 2), half_at(core_from, half)],
                d_send_sem.at[0],
                d_recv.at[spot_from // 2, core_from],
                me,
                1 - core,
            ).wait_recv()

        return carry

    lax.fori_loop(0, plane_size, recv_rows, 0)
    for load in loads:
        load.wait()
    for swap in swaps:
        swap.wait_recv()
    rows = r_buf[...]
    total = None
    for part in range(2):
        gate_value = jnp.dot(rows, gate[part], preferred_element_type=jnp.float32)
        up_value = jnp.dot(rows, up[part], preferred_element_type=jnp.float32)
        expert_hidden = (gate_value * jax.nn.sigmoid(gate_value) * up_value).astype(jnp.bfloat16)
        term = jnp.dot(expert_hidden, down[part], preferred_element_type=jnp.float32)
        total = term if total is None else total + term
    y_send[...] = total.astype(jnp.bfloat16)

    def back_copy(spot_to, core_to, spot_from):
        return remote(
            y_send.at[rows_at(spot_to // 2), half_at(core_to, half)],
            y_buf.at[rows_at(spot_from)],
            y_send_sem.at[spot_to // 2, core_to],
            y_recv.at[spot_from],
            layer * plane_size + spot_to,
            core_to,
        )

    def send_back(n, carry):
        spot_to = spot ^ (2 * (7 - n // 2) + (lax.rem(spot, 2) ^ core))
        core_to = lax.rem(n, 2)

        @pl.when((spot_to != spot) | (core_to != core))
        def _():
            back_copy(spot_to, core_to, spot).start()

        return carry

    lax.fori_loop(0, plane_size, send_back, 0)

    @pl.when(mine)
    def _():
        y_buf[rows_at(spot)] = y_send[rows_at(spot // 2), half_at(core, half)]

    def recv_back(n, carry):
        spot_from = spot ^ n

        @pl.when((spot_from != spot) | jnp.logical_not(mine))
        def _():
            remote(
                y_send.at[rows_at(0), half_at(0, half)],
                y_buf.at[rows_at(spot_from)],
                y_send_sem.at[0, 0],
                y_recv.at[spot_from],
                me,
                1 - core,
            ).wait_recv()

        return carry

    lax.fori_loop(0, plane_size, recv_back, 0)
    p_send[...] = jnp.dot(weighing, y_buf[...], preferred_element_type=jnp.float32).astype(
        jnp.bfloat16
    )
    send_in_column(p_buf, block_at, p_send_sem, p_recv, depth, p_send)
    p_buf[rows_at(layer)] = p_send[rows_at(layer)]
    column_waits(p_buf, block_at, p_send_sem, p_recv, depth, False)
    result = hidden_ref[...].astype(jnp.float32)
    for n in range(depth):
        result = result + p_buf[n * group_rows : (n + 1) * group_rows].astype(jnp.float32)
    out_ref[...] = result.astype(jnp.bfloat16)

    column_waits(table_buf, tile_at, t_send, t_recv, depth, True)
    column_waits(x_buf, block_at, x_send_sem, x_recv, depth, True)
    column_waits(p_buf, block_at, p_send_sem, p_recv, depth, True)
    for swap in swaps:
        swap.wait_send()

    def sent_rows(n, carry):
        @pl.when((n != spot) | jnp.logical_not(mine))
        def _():
            row_copy(n, spot, core).wait_send()

        return carry

    def sent_back(n, carry):
        spot_to = 2 * (n // 2) + core
        core_to = lax.rem(n, 2)

        @pl.when((spot_to != spot) | (core_to != core))
        def _():
            back_copy(spot_to, core_to, spot).wait_send()

        return carry

    lax.fori_loop(0, plane_size, sent_rows, 0)
    lax.fori_loop(0, plane_size, sent_back, 0)


def routed_experts(x_half, own_half, routes, route_weights, w_exp_gate, w_exp_up, w_exp_down):
    depth = lax.axis_size("ep") // plane_size
    half = x_half.shape[1]
    vmem = pl.BlockSpec(memory_space=pltpu.VMEM)
    anywhere = pl.BlockSpec(memory_space=pl.ANY)
    bf16, dma = jnp.bfloat16, pltpu.SemaphoreType.DMA
    rows = plane_size * group_rows
    hidden_half = w_exp_gate.shape[2]
    return pl.pallas_call(
        moe_kernel,
        out_shape=jax.ShapeDtypeStruct(own_half.shape, bf16),
        in_specs=[vmem] * 4 + [anywhere] * 3,
        out_specs=vmem,
        scratch_shapes=[
            pltpu.VMEM((2, 2 * half, hidden_half), bf16),
            pltpu.VMEM((2, 2 * half, hidden_half), bf16),
            pltpu.VMEM((2, hidden_half, 2 * half), bf16),
            pltpu.VMEM((depth, 16, depth * group_rows), jnp.float32),
            pltpu.VMEM((depth * group_rows, half), bf16),
            pltpu.VMEM((rows, half), bf16),
            pltpu.VMEM((rows // 2, 2 * half), bf16),
            pltpu.VMEM((rows // 2, 2 * half), bf16),
            pltpu.VMEM((rows, half), bf16),
            pltpu.VMEM((depth * group_rows, half), bf16),
            pltpu.VMEM((depth * group_rows, half), bf16),
            dma((3,)),
            dma((3,)),
            dma((3,)),
            dma((depth,)),
            dma((depth,)),
            dma((depth,)),
            dma((depth,)),
            dma((plane_size,)),
            dma((plane_size // 2, 2)),
            dma((plane_size // 2, 2)),
            dma((plane_size,)),
            dma((depth,)),
            dma((depth,)),
        ],
        compiler_params=pltpu.CompilerParams(collective_id=0, has_side_effects=True),
    )(x_half, own_half, routes.T, route_weights.T, w_exp_gate, w_exp_up, w_exp_down)


def local(
    tokens,
    lengths,
    lat_cache,
    rope_cache,
    norm1_gain,
    w_qdown,
    w_kvdown,
    w_kdown_rope,
    qnorm_gain,
    kvnorm_gain,
    w_qup_nope,
    w_qup_rope,
    w_absorb_k,
    w_absorb_v,
    w_attn_out,
    norm2_gain,
    routes,
    route_weights,
    w_exp_gate,
    w_exp_up,
    w_exp_down,
):
    score_scale = (w_qup_nope.shape[2] + w_qup_rope.shape[2]) ** (-0.5)
    core_index = lax.axis_index("tp")
    group_rows = tokens.shape[0]
    own_rows = lat_cache.shape[0]
    full_tokens = gather_directly(tokens, "tp", 1)
    token_values = full_tokens.astype(jnp.float32)
    model_width = full_tokens.shape[1]
    half_width = tokens.shape[1]
    normed1 = rms_scale(token_values, norm1_gain).astype(jnp.bfloat16)
    feature_rows = w_qdown.shape[0]
    local_rows = lax.dynamic_slice_in_dim(normed1, core_index * feature_rows, feature_rows, 1)
    query_low, kv_low, rope_low = in_one(
        (
            jnp.dot(local_rows, w_qdown, preferred_element_type=jnp.float32),
            jnp.dot(local_rows, w_kvdown, preferred_element_type=jnp.float32),
            jnp.dot(local_rows, w_kdown_rope, preferred_element_type=jnp.float32),
        ),
        "tp",
    )
    compressed = rms_scale(query_low, qnorm_gain).astype(jnp.bfloat16)
    latent_all = rms_scale(kv_low, kvnorm_gain).astype(jnp.bfloat16)
    rope_all = rotate(rope_low, lengths).astype(jnp.bfloat16)
    query_nope = jnp.einsum(
        "sc,chd->shd", compressed, w_qup_nope, preferred_element_type=jnp.float32
    ).astype(jnp.bfloat16)
    rope_part = jnp.einsum(
        "sc,chd->shd", compressed, w_qup_rope, preferred_element_type=jnp.float32
    )
    query_rope = (rotate(rope_part, lengths) * score_scale).astype(jnp.bfloat16)
    query_latent = (
        jnp.einsum("shd,hdc->shc", query_nope, w_absorb_k, preferred_element_type=jnp.float32)
        * score_scale
    ).astype(jnp.bfloat16)
    seq_latent, seq_rope = sent_together((query_latent, query_rope), "tp", 0, 1, 2)
    first_row = core_index * own_rows
    new_latent = lax.dynamic_slice_in_dim(latent_all, first_row, own_rows, 0)
    new_rope_key = lax.dynamic_slice_in_dim(rope_all, first_row, own_rows, 0)
    own_lengths = lax.dynamic_slice_in_dim(lengths, first_row, own_rows, 0)
    attended = attend(
        seq_latent, seq_rope, lat_cache, rope_cache, new_latent, new_rope_key, own_lengths
    )
    head_latent = lax.all_to_all(attended, "tp", split_axis=1, concat_axis=0, tiled=True)
    head_out = jnp.einsum(
        "shc,hcv->shv", head_latent, w_absorb_v, preferred_element_type=jnp.float32
    ).astype(jnp.bfloat16)
    attention_sum = over_copies(
        jnp.einsum("shv,hvd->sd", head_out, w_attn_out, preferred_element_type=jnp.float32), "tp"
    )
    hidden1 = (token_values + attention_sum).astype(jnp.bfloat16)
    normed2 = rms_scale(hidden1.astype(jnp.float32), norm2_gain).astype(jnp.bfloat16)
    own_half = lax.dynamic_slice_in_dim(hidden1, core_index * half_width, half_width, 1)
    normed2_half = lax.dynamic_slice_in_dim(normed2, core_index * half_width, half_width, 1)
    mixed = routed_experts(
        normed2_half, own_half, routes, route_weights, w_exp_gate, w_exp_up, w_exp_down
    )
    return (mixed, new_latent, new_rope_key)


def solution(mesh):
    return jax.shard_map(
        local,
        mesh=mesh,
        in_specs=(
            P("ep", "tp"),
            P("ep"),
            P(("ep", "tp"), None, None),
            P(("ep", "tp"), None, None),
            P(),
            P("tp", None),
            P("tp", None),
            P("tp", None),
            P(),
            P(),
            P(None, "tp", None),
            P(None, "tp", None),
            P("tp", None, None),
            P("tp", None, None),
            P("tp", None, None),
            P(),
            P("ep", None),
            P("ep", None),
            P("ep", None, "tp"),
            P("ep", None, "tp"),
            P("ep", "tp", None),
        ),
        out_specs=(P("ep", "tp"), P(("ep", "tp"), None), P(("ep", "tp"), None)),
        check_vma=False,
    )
```
